32 devices in a mesh: grp: 1, ep: 16 (over z, y, x), tp: 2 (over core).
Axes of the slice: x: 2, y: 2, z: 4, core: 2. Of those that a mesh axis runs over, the one named last changes fastest.
Arguments:
- tokens: bfloat16 [2048, 2048], P(('grp', 'ep', 'tp')), may hold values from -6 to 6
- norm_gain: float32 [2048], replicated, may hold values from 0.1 to 1.9
- expert_ids: int32 [2048, 2], P(('grp', 'ep', 'tp')), may hold values from 0 to 3, all different within a row; in each aligned block of 64 rows (0 to 63, 64 to 127, ...) at most 42 rows name the same one
- gate_weights: float32 [2048, 2], P(('grp', 'ep', 'tp')), may hold values from 0.2 to 1
- w_gate: bfloat16 [2048, 28672], P(None, ('ep', 'tp')), may hold values from -0.125 to 0.125
- w_up: bfloat16 [2048, 28672], P(None, ('ep', 'tp')), may hold values from -0.125 to 0.125
- w_down: bfloat16 [28672, 2048], P(('ep', 'tp')), may hold values from -0.0625 to 0.0625
Outputs:
- mixed: bfloat16 [2048, 2048], P(('grp', 'ep', 'tp'))
The draws below stay inside these ranges and needn't reach their ends.
Inputs may be any that keep to these rules, and one draw needn't show every extreme that they name: `expert_ids`: each token names 2 different experts. Among the rows of one device no expert is named by more than 42 rows, a bound that some blocks reach; every expert is named somewhere.
All inputs are finite; a program needn't handle non-finite values.
Results may differ from the reference program's by a relative error of at most 0.0095.
Values may be sent and summed in bfloat16 or wider, within the bound.
No kernel may reach another device: no remote copies, remote signals or barrier semaphores. Data moves between devices by JAX's collectives and lax.ppermute only.
A program may use at most 192 MiB of HBM per device.

```python
import math
import jax
import jax.numpy as jnp
import numpy as np
from jax import lax

D = 2048
FF = 7168
TOPK = 2
GROUP = 4
TOK_DEV = 64
EXPERTS = 4
CAP = 42
TOKENS = 2048
N_EP = 16
N_TP = 2


def steps_of(own_key, shape, pieces, low, largest):
    level = 1.0
    for dim, shards_of in pieces:
        heights = jax.random.uniform(jax.random.fold_in(jax.random.fold_in(own_key, 6), dim), (shards_of,), jnp.float32, low / len(pieces), largest / len(pieces))
        level = level * jnp.repeat(jnp.exp(heights), shape[dim] // shards_of).reshape((-1,) + (1,) * (len(shape) - 1 - dim))
    return level


def routed_block(stream_key, own, number, rows, amount, top, limit, lean):
    ranking = jax.random.permutation(stream_key, amount)
    crowded, common = load_shares(amount, rows * top, limit, lean, True), load_shares(amount, rows * top, limit, lean, False)
    places = jnp.arange(amount)

    def named(lengths, turn):
        used = int((lengths > 0).sum())
        fixed = max(1, used // 4)
        passed = fixed + (places - fixed + turn * (used - fixed)) % max(1, amount - fixed)
        return jnp.zeros((amount,), jnp.int32).at[ranking[jnp.where(places < fixed, places, passed)]].set(jnp.asarray(lengths, jnp.int32))

    lengths = jnp.where(number % 4 == 0, named(crowded, number // 4), named(common, number - number // 4 - 1))
    mixed = jax.random.permutation(jax.random.fold_in(own, 3), amount)
    source_of, sink = mixed[0:amount // 2 * 2:2], mixed[1:amount // 2 * 2:2]
    room = jnp.minimum(lengths[source_of] - 1, limit - lengths[sink]) // 2
    room = jnp.where((source_of == ranking[0]) | (sink == ranking[0]) | (lengths[sink] == 0), 0, jnp.maximum(room, 0))
    passed = jax.random.randint(jax.random.fold_in(own, 4), (amount // 2,), 0, 1 << 20) % (room + 1)
    lengths = lengths.at[source_of].add(-passed).at[sink].add(passed)
    members = jnp.searchsorted(jnp.cumsum(lengths), jnp.arange(rows * top), side="right").astype(jnp.int32)
    table = members.reshape(top, rows).T
    table = table[jax.random.permutation(jax.random.fold_in(own, 1), rows)]
    turn = jax.random.randint(jax.random.fold_in(own, 2), (rows, 1), 0, top)
    return jnp.take_along_axis(table, (jnp.arange(top)[None, :] + turn) % top, axis=1)


def load_shares(count, total, bound, slope, full):
    portions = [(1 << 20) // math.isqrt(standing ** slope) + 1 for standing in range(1, count + 1)]
    largest = bound if full else min(bound, max(-(-total // count), total * portions[0] // sum(portions)))
    least = 1 if total - largest >= count - 1 else 0
    counts, spare = [largest] + [least] * (count - 1), total - largest - least * (count - 1)
    while spare > 0:
        free = [i for i in range(1, count) if counts[i] < largest] or [i for i in range(1, count) if counts[i] < bound]
        whole, left = sum([portions[i] for i in free]), spare
        for i in free:
            addition = min(bound - counts[i], max(1, left * portions[i] // whole), spare)
            counts[i] = counts[i] + addition
            spare = spare - addition
    return np.array(counts)


def gaussian(rng, dims, scale, bound, shards=(), kind=jnp.bfloat16):
    gain = steps_of(rng, dims, shards, -0.22, 0.18) if shards else 1.0
    result = jax.random.normal(rng, dims, jnp.float32) * scale * gain
    return jnp.minimum(jnp.maximum(result, -bound), bound).astype(kind)


def setup_inputs(seed: int = 0, part: int = 0) -> dict:
    key_of = jax.random.split(jax.random.key(seed), 8)
    part_splits = jax.random.split(jax.random.fold_in(key_of[7], part), 8)
    tokens = gaussian(part_splits[0], (TOKENS, D), 1.0, 6.0, ((0, 32),))
    norm_gain = jnp.clip(1.0 + 0.18 * jax.random.normal(key_of[1], (D,), jnp.float32), 0.1, 1.9)
    expert_ids_keys = jax.random.split(jax.random.fold_in(part_splits[2], 1), TOKENS // TOK_DEV)
    expert_ids_turns = jax.random.permutation(jax.random.fold_in(part_splits[2], 3), TOKENS // TOK_DEV)
    expert_ids = jax.vmap(lambda own, number: routed_block(jax.random.fold_in(part_splits[2], 2), own, number, TOK_DEV, EXPERTS, TOPK, CAP, 2))(expert_ids_keys, expert_ids_turns).reshape((TOKENS, TOPK))
    gate_weights = jnp.clip(0.2 + 0.8 * jax.random.uniform(part_splits[3], (TOKENS, TOPK), jnp.float32) ** steps_of(part_splits[3], (TOKENS, TOPK), ((0, 32),), -0.2, 0.2), 0.2, 1.0)
    w_gate = gaussian(key_of[4], (D, EXPERTS * FF), D ** -0.5, 0.125, ((1, 32),))
    w_up = gaussian(key_of[5], (D, EXPERTS * FF), D ** -0.5, 0.125, ((1, 32),))
    w_down = gaussian(key_of[6], (EXPERTS * FF, D), FF ** -0.5, 0.0625, ((0, 32),))
    return {"tokens": tokens, "norm_gain": norm_gain, "expert_ids": expert_ids, "gate_weights": gate_weights, "w_gate": w_gate, "w_up": w_up, "w_down": w_down}


def layer_norm(tokens, norm_gain):
    values = tokens.astype(jnp.float32)
    center = lax.optimization_barrier(jnp.mean(values, -1, keepdims=True))
    spread = lax.optimization_barrier(jnp.mean(jnp.square(values - center), -1, keepdims=True))
    return ((values - center) * lax.rsqrt(spread + 1e-05) * norm_gain).astype(jnp.bfloat16)

def rounded(values):
    return lax.optimization_barrier(values.astype(jnp.bfloat16)).astype(jnp.float32)

def reference(tokens, norm_gain, expert_ids, gate_weights, w_gate, w_up, w_down):
    normed = layer_norm(tokens, norm_gain)
    padded = jnp.concatenate([normed, jnp.zeros((1, D), jnp.bfloat16)], 0)
    flat_ids = expert_ids.reshape(-1).astype(jnp.int32)
    matches = (flat_ids[:, None] == jnp.arange(EXPERTS, dtype=jnp.int32)[None, :]).astype(jnp.int32)
    position = lax.optimization_barrier(jnp.sum((jnp.cumsum(matches, 0) - 1) * matches, 1)).astype(jnp.int32)
    buffer_rows = N_EP * N_TP * CAP
    source = (jnp.arange(TOKENS * TOPK, dtype=jnp.int32) // TOPK).astype(jnp.int32)
    slot_table = jnp.full((EXPERTS, buffer_rows), TOKENS, jnp.int32).at[flat_ids, position].set(source)
    block_width = FF // (GROUP * N_TP)

    def one_expert(expert_index):
        picked_rows = padded[slot_table[expert_index]]
        first_col = (expert_index * FF).astype(jnp.int32)
        gate_cols = lax.dynamic_slice_in_dim(w_gate, first_col, FF, 1)
        up_cols = lax.dynamic_slice_in_dim(w_up, first_col, FF, 1)
        down_rows = lax.dynamic_slice_in_dim(w_down, first_col, FF, 0)
        running = jnp.zeros((buffer_rows, D), jnp.float32)
        for member in range(GROUP):
            paired = jnp.zeros((buffer_rows, D), jnp.float32)
            for side_index in range(N_TP):
                offset = (member * N_TP + side_index) * block_width
                gate_part = jnp.dot(picked_rows, gate_cols[:, offset:offset + block_width], preferred_element_type=jnp.float32)
                up_part = jnp.dot(picked_rows, up_cols[:, offset:offset + block_width], preferred_element_type=jnp.float32)
                hidden_part = (jax.nn.silu(gate_part) * up_part).astype(jnp.bfloat16)
                paired = paired + rounded(jnp.dot(hidden_part, down_rows[offset:offset + block_width], preferred_element_type=jnp.float32))
            running = running + rounded(paired)
        return running
    results = lax.map(one_expert, jnp.arange(EXPERTS, dtype=jnp.int32))
    picked = results[flat_ids, position] * gate_weights.reshape(-1)[:, None]
    return lax.optimization_barrier(jnp.sum(picked.reshape(TOKENS, TOPK, D), 1)).astype(jnp.bfloat16)
```

```python
import functools

import jax
import jax.numpy as jnp
from jax import lax
from jax.experimental import pallas as pl
from jax.experimental.pallas import tpu as pltpu
from jax.sharding import PartitionSpec as P

GROUP = 4
PIECES = 8
VMEM = pltpu.MemorySpace.VMEM
SMEM = pltpu.MemorySpace.SMEM


def slots(ids, me, experts, width):
    rows = ids.shape[0]
    lanes = lax.broadcasted_iota(jnp.int32, (rows, 128), 1) ^ me
    hits = (ids[:, 0:1] == lanes) | (ids[:, 1:2] == lanes)
    hits = jnp.where(hits, 1.0, 0.0).astype(jnp.bfloat16)
    token = lax.broadcasted_iota(jnp.int32, (rows, width), 1) % rows
    own = lax.broadcasted_iota(jnp.int32, (rows, width), 0)
    before = jnp.where(own < token, 1.0, 0.0).astype(jnp.bfloat16)
    same = jnp.where(own == token, 1.0, 0.0).astype(jnp.bfloat16)
    dims = (((0,), (0,)), ((), ()))
    place = lax.dot_general(hits, before, dims, preferred_element_type=jnp.float32)
    chosen = lax.dot_general(hits, same, dims, preferred_element_type=jnp.float32)
    return jnp.where(chosen > 0.5, place, -1.0e6).astype(jnp.int32)


def pack_kernel(experts, cap, me_ref, tokens_ref, gain_ref, ids_ref, *rest):
    outs, stacked = rest[:-1], rest[-1]
    rows, width = tokens_ref.shape
    piece = width // PIECES
    values = tokens_ref[...].astype(jnp.float32)
    center = jnp.mean(values, -1, keepdims=True)
    values = values - center
    spread = jnp.mean(jnp.square(values), -1, keepdims=True)
    normed = (values * lax.rsqrt(spread + 1e-05) * gain_ref[...]).astype(jnp.bfloat16)
    for p in range(PIECES):
        stacked[p * rows : (p + 1) * rows, :] = normed[:, p * piece : (p + 1) * piece]
    span = PIECES * rows
    place = slots(ids_ref[...], me_ref[0], experts, span)
    place = place + lax.broadcasted_iota(jnp.int32, place.shape, 1) // rows * cap
    out_row = lax.broadcasted_iota(jnp.int32, (PIECES * cap, span), 0)
    for k in range(experts):
        pick = jnp.where(out_row == place[k : k + 1, :], 1.0, 0.0).astype(jnp.bfloat16)
        outs[k][...] = jnp.dot(pick, stacked[...], preferred_element_type=jnp.float32).astype(jnp.bfloat16)


def pack(me, tokens, gain, ids, experts, cap):
    rows, width = tokens.shape
    block = jax.ShapeDtypeStruct((PIECES * cap, width // PIECES), jnp.bfloat16)
    return pl.pallas_call(
        functools.partial(pack_kernel, experts, cap),
        out_shape=[block] * experts,
        in_specs=[pl.BlockSpec(memory_space=SMEM)] + [pl.BlockSpec(memory_space=VMEM)] * 3,
        out_specs=[pl.BlockSpec(memory_space=VMEM)] * experts,
        scratch_shapes=[pltpu.VMEM((PIECES * rows, width // PIECES), jnp.bfloat16)],
        cost_estimate=pl.CostEstimate(flops=1_000_000_000, bytes_accessed=1_000_000, transcendentals=0),
        name="pack",
    )(me, tokens, gain.reshape(1, -1), ids)


def cuts(size, largest):
    return [(at, min(largest, size - at)) for at in range(0, size, largest)]


def ffn_kernel(n_tp, cap, pad, *refs):
    gates, ups, downs = refs[:n_tp], refs[n_tp : 2 * n_tp], refs[2 * n_tp : 3 * n_tp]
    own, from_x, from_y, diag_a, diag_b = refs[3 * n_tp : 3 * n_tp + 5]
    out_own, out_x, out_y, out_a, out_b = refs[3 * n_tp + 5 : 3 * n_tp + 10]
    gate, up, down, x, h, sems = refs[3 * n_tp + 10 :]
    width, part = gates[0].shape
    hidden = part * n_tp
    piece = width // PIECES
    half = PIECES // 2 * cap
    blocks = own.shape[0]

    first, second, sem = [], [], 0
    for c in range(n_tp):
        for at, size in cuts(part, 512):
            here = pl.ds(at, size)
            there = pl.ds(c * part + at, size)
            pair = []
            for source, target in ((gates[c], gate), (ups[c], up)):
                copy = pltpu.make_async_copy(source.at[:, here], target.at[:, there], sems.at[sem])
                sem += 1
                copy.start()
                pair.append(copy)
            first.append((c * part + at, pair))
    for at, size in cuts(width, 512):
        pair = []
        for c in range(n_tp):
            copy = pltpu.make_async_copy(
                downs[c].at[:, pl.ds(at, size)], down.at[pl.ds(c * part, part), pl.ds(at, size)], sems.at[sem]
            )
            sem += 1
            copy.start()
            pair.append(copy)
        second.append((at, pair))

    def arrived(waiting, end):
        while waiting and waiting[0][0] < end:
            for copy in waiting.pop(0)[1]:
                copy.wait()

    for b in range(blocks):
        for m, buf in enumerate((own, from_x, from_y)):
            row = (m * blocks + b) * pad
            for p in range(PIECES):
                x[row : row + cap, p * piece : (p + 1) * piece] = buf[b, p * cap : (p + 1) * cap, :]
        row = (3 * blocks + b) * pad
        for p in range(PIECES):
            buf, q = (diag_a, p) if p < PIECES // 2 else (diag_b, p - PIECES // 2)
            x[row : row + cap, p * piece : (p + 1) * piece] = buf[b, q * cap : (q + 1) * cap, :]

    for at, size in cuts(hidden, 256):
        arrived(first, at + size)
        g = jnp.dot(x[...], gate[:, at : at + size], preferred_element_type=jnp.float32)
        u = jnp.dot(x[...], up[:, at : at + size], preferred_element_type=jnp.float32)
        h[:, at : at + size] = (g * jax.nn.sigmoid(g) * u).astype(jnp.bfloat16)
    for p in range(PIECES):
        arrived(second, (p + 1) * piece)
        term = jnp.dot(h[...], down[:, p * piece : (p + 1) * piece], preferred_element_type=jnp.float32)
        for b in range(blocks):
            for m, out in enumerate((out_own, out_x, out_y)):
                row = (m * blocks + b) * pad
                out[b, p * cap : (p + 1) * cap, :] = term[row : row + cap]
            row = (3 * blocks + b) * pad
            out, q = (out_a, p) if p < PIECES // 2 else (out_b, p - PIECES // 2)
            out[b, q * cap : (q + 1) * cap, :] = term[row : row + cap].astype(jnp.bfloat16)


def ffn(gates, ups, downs, own, from_x, from_y, diag_a, diag_b, cap):
    n_tp = len(gates)
    width, part = gates[0].shape
    blocks = own.shape[0]
    pad = -(-cap // 16) * 16
    rows = GROUP * blocks * pad
    hidden = part * n_tp
    piece = width // PIECES
    whole = jax.ShapeDtypeStruct((blocks, PIECES * cap, piece), jnp.float32)
    halves = jax.ShapeDtypeStruct((blocks, PIECES // 2 * cap, piece), jnp.bfloat16)
    copies = n_tp * (2 * len(cuts(part, 512)) + len(cuts(width, 512)))
    return pl.pallas_call(
        functools.partial(ffn_kernel, n_tp, cap, pad),
        out_shape=[whole] * 3 + [halves] * 2,
        in_specs=[pl.BlockSpec(memory_space=pl.ANY)] * (3 * n_tp) + [pl.BlockSpec(memory_space=VMEM)] * 5,
        out_specs=[pl.BlockSpec(memory_space=VMEM)] * 5,
        scratch_shapes=[
            pltpu.VMEM((width, hidden), jnp.bfloat16),
            pltpu.VMEM((width, hidden), jnp.bfloat16),
            pltpu.VMEM((hidden, width), jnp.bfloat16),
            pltpu.VMEM((rows, width), jnp.bfloat16),
            pltpu.VMEM((rows, hidden), jnp.bfloat16),
            pltpu.SemaphoreType.DMA((copies,)),
        ],
        compiler_params=pltpu.CompilerParams(vmem_limit_bytes=40 * 1024 * 1024),
        cost_estimate=pl.CostEstimate(
            flops=6 * rows * width * hidden, bytes_accessed=6 * width * hidden, transcendentals=rows * hidden
        ),
        name="ffn",
    )(*gates, *ups, *downs, own, from_x, from_y, diag_a, diag_b)


def add_kernel(half, x_ref, y_ref, a_ref, b_ref, x_out, y_out):
    x_out[:, :half, :] = x_ref[:, :half, :].astype(jnp.bfloat16)
    x_out[:, half:, :] = (x_ref[:, half:, :] + b_ref[...].astype(jnp.float32)).astype(jnp.bfloat16)
    y_out[:, :half, :] = (y_ref[:, :half, :] + a_ref[...].astype(jnp.float32)).astype(jnp.bfloat16)
    y_out[:, half:, :] = y_ref[:, half:, :].astype(jnp.bfloat16)


def add_diag(x_part, y_part, got_a, got_b):
    half = got_a.shape[1]
    shape = jax.ShapeDtypeStruct(x_part.shape, jnp.bfloat16)
    return pl.pallas_call(
        functools.partial(add_kernel, half),
        out_shape=[shape, shape],
        in_specs=[pl.BlockSpec(memory_space=VMEM)] * 4,
        out_specs=[pl.BlockSpec(memory_space=VMEM)] * 2,
        cost_estimate=pl.CostEstimate(flops=100_000_000, bytes_accessed=1_000_000, transcendentals=0),
        name="add_diag",
    )(x_part, y_part, got_a, got_b)


def combine_kernel(experts, cap, pad, me_ref, ids_ref, weights_ref, *rest):
    parts, out_ref, gathered = rest[:experts], rest[experts], rest[experts + 1]
    rows, width = out_ref.shape
    piece = width // PIECES
    gathered[...] = jnp.zeros_like(gathered)
    for k in range(experts):
        for p in range(PIECES):
            gathered[k * pad : k * pad + cap, p * piece : (p + 1) * piece] = parts[k][p * cap : (p + 1) * cap, :]
    ids, me = ids_ref[...], me_ref[0]
    lanes = lax.broadcasted_iota(jnp.int32, (rows, 128), 1) ^ me
    hits = jnp.where((ids[:, 0:1] == lanes) | (ids[:, 1:2] == lanes), 1.0, 0.0).astype(jnp.bfloat16)
    before = lax.broadcasted_iota(jnp.int32, (rows, rows), 1) < lax.broadcasted_iota(jnp.int32, (rows, rows), 0)
    before = jnp.where(before, 1.0, 0.0).astype(jnp.bfloat16)
    place = jnp.dot(before, hits, preferred_element_type=jnp.float32)
    total = jnp.zeros((rows, width), jnp.float32)
    column = lax.broadcasted_iota(jnp.int32, (rows, experts * pad), 1)
    for pick in range(2):
        mine = ids[:, pick : pick + 1] == lanes
        lane = lax.broadcasted_iota(jnp.int32, (rows, 128), 1)
        slot = jnp.where(mine, place + (lane * pad).astype(jnp.float32), 0.0)
        slot = jnp.sum(slot, -1, keepdims=True).astype(jnp.int32)
        onehot = jnp.where(column == slot, 1.0, 0.0).astype(jnp.bfloat16)
        chosen = jnp.dot(onehot, gathered[...], preferred_element_type=jnp.float32)
        total = total + chosen * weights_ref[:, pick : pick + 1]
    out_ref[...] = total.astype(jnp.bfloat16)


def combine(me, ids, weights, parts, cap, width):
    experts, rows = len(parts), ids.shape[0]
    pad = -(-cap // 16) * 16
    return pl.pallas_call(
        functools.partial(combine_kernel, experts, cap, pad),
        out_shape=jax.ShapeDtypeStruct((rows, width), jnp.bfloat16),
        in_specs=[pl.BlockSpec(memory_space=SMEM)] + [pl.BlockSpec(memory_space=VMEM)] * (2 + experts),
        out_specs=pl.BlockSpec(memory_space=VMEM),
        scratch_shapes=[pltpu.VMEM((experts * pad, width), jnp.bfloat16)],
        cost_estimate=pl.CostEstimate(flops=1_000_000_000, bytes_accessed=1_000_000, transcendentals=0),
        name="combine",
    )(me, ids, weights, *parts)


def per_device(tokens, norm_gain, expert_ids, gate_weights, w_gate, w_up, w_down):
    ep_devices, n_tp = lax.axis_size("ep"), lax.axis_size("tp")
    local_rows, width = tokens.shape
    picks = expert_ids.shape[1]
    experts = ep_devices // GROUP
    cap = max(2, min(local_rows, local_rows * picks * 4 // (3 * experts)))
    half = PIECES // 2 * cap

    def flip(value, bits):
        return lax.ppermute(value, "ep", [(i, i ^ bits) for i in range(ep_devices)])

    def across(value):
        turns = [[(i, (i + s) % n_tp) for i in range(n_tp)] for s in range(1, n_tp)]
        return [value] + [lax.ppermute(value, "tp", turn) for turn in turns]

    me = (lax.axis_index("ep") // GROUP).astype(jnp.int32).reshape(1)
    blocks = pack(me, tokens, norm_gain, expert_ids, experts, cap)
    gates, ups, downs = across(w_gate), across(w_up), across(w_down)
    arrived = [blocks[0]] + [flip(blocks[k], k * GROUP) for k in range(1, experts)]

    chunks = min(4, experts)
    size = experts // chunks
    returned = [None] * experts
    for g in range(chunks):
        own = jnp.stack(arrived[g * size : (g + 1) * size])
        from_x, from_y = flip(own, 1), flip(own, 2)
        diag_a, diag_b = flip(from_x[:, :half], 2), flip(from_y[:, half:], 1)
        mine, to_x, to_y, to_a, to_b = ffn(gates, ups, downs, own, from_x, from_y, diag_a, diag_b, cap)
        got_a, got_b = flip(to_a, 1), flip(to_b, 2)
        send_x, send_y = add_diag(to_x, to_y, got_a, got_b)
        got_x, got_y = flip(send_x, 1), flip(send_y, 2)
        total = mine + got_x.astype(jnp.float32) + got_y.astype(jnp.float32)
        total = total.astype(jnp.bfloat16)
        for j in range(size):
            k = g * size + j
            returned[k] = flip(total[j], k * GROUP) if k else total[j]
    return combine(me, expert_ids, gate_weights, returned, cap, width)


def solution(mesh):
    in_specs = (
        P(("grp", "ep", "tp"), None),
        P(),
        P(("grp", "ep", "tp"), None),
        P(("grp", "ep", "tp"), None),
        P(None, ("ep", "tp")),
        P(None, ("ep", "tp")),
        P(("ep", "tp"), None),
    )
    out_specs = P(("grp", "ep", "tp"), None)
    return jax.shard_map(
        per_device, mesh=mesh, in_specs=in_specs, out_specs=out_specs, check_vma=False
    )
```

```python
import functools

import jax
import jax.numpy as jnp
from jax import lax
from jax.experimental import pallas as pl
from jax.experimental.pallas import tpu as pltpu
from jax.sharding import PartitionSpec as P


GROUP = 4
PIECES = 8
TAKE = ((0,), (1,), (2,), (3,))
WORK = ((3,), (2,), (1,), (0,))
GIVE = ((3,), (2,), (1,), (0,))
FFN_VMEM = 5 * 1024 * 1024
LOAD_VMEM = 5 * 1024 * 1024
PACK_VMEM = 63 * 1024 * 1024
SMALL_VMEM = 10 * 1024 * 1024
VMEM = pltpu.MemorySpace.VMEM
SMEM = pltpu.MemorySpace.SMEM


def pack_kernel(experts, cap, me_ref, tokens_ref, gain_ref, ids_ref, *rest):
    outs, stacked = rest[:-1], rest[-1]
    rows, width = tokens_ref.shape
    piece = width // PIECES
    values = tokens_ref[...].astype(jnp.float32)
    center = jnp.mean(values, -1, keepdims=True)
    values = values - center
    spread = jnp.mean(jnp.square(values), -1, keepdims=True)
    normed = (values * lax.rsqrt(spread + 1e-05) * gain_ref[...]).astype(jnp.bfloat16)
    for p in range(PIECES):
        stacked[p * rows : (p + 1) * rows, :] = normed[:, p * piece : (p + 1) * piece]
    span = PIECES * rows
    place = places(ids_ref[...], me_ref[0], experts, span)
    place = place + lax.broadcasted_iota(jnp.int32, place.shape, 1) // rows * cap
    out_row = lax.broadcasted_iota(jnp.int32, (PIECES * cap, span), 0)
    for k in range(experts):
        pick = jnp.where(out_row == place[k : k + 1, :], 1.0, 0.0).astype(jnp.bfloat16)
        outs[k][...] = jnp.dot(pick, stacked[...], preferred_element_type=jnp.float32).astype(jnp.bfloat16)


def places(ids, me, experts, width):
    rows = ids.shape[1]
    count = -(-experts // 16) * 16
    expert = lax.broadcasted_iota(jnp.int32, (count, rows), 0) ^ me
    hits = (ids[0:1, :] == expert) | (ids[1:2, :] == expert)
    hits = jnp.where(hits, 1.0, 0.0).astype(jnp.bfloat16)
    token = lax.broadcasted_iota(jnp.int32, (rows, width), 1) % rows
    own = lax.broadcasted_iota(jnp.int32, (rows, width), 0)
    before = jnp.where(own < token, 1.0, 0.0).astype(jnp.bfloat16)
    same = jnp.where(own == token, 1.0, 0.0).astype(jnp.bfloat16)
    place = jnp.dot(hits, before, preferred_element_type=jnp.float32)
    chosen = jnp.dot(hits, same, preferred_element_type=jnp.float32)
    return jnp.where(chosen > 0.5, place, -1.0e6).astype(jnp.int32)


def pack(me, tokens, gain, ids, experts, cap):
    rows, width = tokens.shape
    block = jax.ShapeDtypeStruct((PIECES * cap, width // PIECES), jnp.bfloat16)
    return pl.pallas_call(
        functools.partial(pack_kernel, experts, cap),
        out_shape=[block] * experts,
        in_specs=[pl.BlockSpec(memory_space=SMEM)] + [pl.BlockSpec(memory_space=VMEM)] * 3,
        out_specs=[pl.BlockSpec(memory_space=VMEM)] * experts,
        scratch_shapes=[pltpu.VMEM((PIECES * rows, width // PIECES), jnp.bfloat16)],
        cost_estimate=pl.CostEstimate(flops=1_000_000_000, bytes_accessed=1_000_000, transcendentals=0),
        compiler_params=pltpu.CompilerParams(vmem_limit_bytes=PACK_VMEM),
        name="pack",
    )(me, tokens, gain.reshape(1, -1), ids)


def cuts(size, largest):
    return [(at, min(largest, size - at)) for at in range(0, size, largest)]


def load_copies(gates, ups, downs, gate, up, down, sems, base):
    first, second, sem = [], [], 0
    width, part = gates[0].shape
    for c in range(len(gates)):
        at = (base + c) * part
        for begin, size in cuts(part, 256):
            here, there = pl.ds(begin, size), pl.ds(at + begin, size)
            pair = []
            for source, target in ((gates[c], gate), (ups[c], up)):
                pair.append(pltpu.make_async_copy(source.at[:, here], target.at[:, there], sems.at[sem]))
                sem += 1
            first.append((at + begin, pair))
    for begin, size in cuts(width, 512):
        here = pl.ds(begin, size)
        pair = []
        for c in range(len(gates)):
            there = pl.ds((base + c) * part, part)
            pair.append(pltpu.make_async_copy(downs[c].at[:, here], down.at[there, here], sems.at[sem]))
            sem += 1
        second.append((begin, pair))
    for _, pair in first + second:
        for copy in pair:
            copy.start()
    return first, second


def copy_count(cores, width, part):
    return cores * (2 * len(cuts(part, 256)) + len(cuts(width, 512)))


def load_kernel(gate_in, up_in, down_in, gate, up, down, sems):
    first, second = load_copies([gate_in], [up_in], [down_in], gate, up, down, sems, 0)
    for _, pair in first + second:
        for copy in pair:
            copy.wait()


HBM_SPEC = pl.BlockSpec(memory_space=pltpu.MemorySpace.HBM)
VMEM_SPEC = pl.BlockSpec(memory_space=VMEM)


def load(gate, up, down, n_tp):
    width, part = gate.shape
    wide = jax.ShapeDtypeStruct((width, n_tp * part), jnp.bfloat16)
    return pl.pallas_call(
        load_kernel,
        out_shape=[wide, wide, jax.ShapeDtypeStruct((n_tp * part, width), jnp.bfloat16)],
        in_specs=[HBM_SPEC] * 3,
        out_specs=[VMEM_SPEC] * 3,
        scratch_shapes=[pltpu.SemaphoreType.DMA((copy_count(1, width, part),))],
        compiler_params=pltpu.CompilerParams(vmem_limit_bytes=LOAD_VMEM),
        cost_estimate=pl.CostEstimate(flops=3_000_000_000, bytes_accessed=12 * width * part, transcendentals=0),
        name="load",
    )(gate, up, down)


def ffn_kernel(cap, counts, cores, *refs):
    refs = list(refs)

    def take(count):
        taken = refs[:count]
        del refs[:count]
        return taken

    whole = take(3)
    if cores:
        gates, ups, downs = take(cores), take(cores), take(cores)
    takes = [take(3) for _ in counts]
    gives = [take(3) for _ in counts]
    if cores:
        whole = take(3)
    gate, up, down = whole
    x, h = take(2)
    width, hidden = gate.shape
    piece = width // PIECES
    blocks = sum(counts)

    first, second = [], []
    if cores:
        (sems,) = take(1)
        first, second = load_copies(gates, ups, downs, gate, up, down, sems, 1)

    def arrived(waiting, end):
        while waiting and waiting[0][0] < end:
            for copy in waiting.pop(0)[1]:
                copy.wait()

    def rows_of(groups):
        base = 0
        for count, (own, near, far) in zip(counts, groups):
            for m, (ref, skip) in enumerate([(own, 0), (near, 0), (far, 0), (far, count)]):
                for b in range(count):
                    yield (m * blocks + base + b) * cap, ref, skip + b
            base += count

    for row, ref, b in rows_of(takes):
        for p in range(PIECES):
            x[row : row + cap, p * piece : (p + 1) * piece] = ref[b, p * cap : (p + 1) * cap, :]

    for at, size in cuts(hidden, 256):
        arrived(first, at + size)
        g = jnp.dot(x[...], gate[:, at : at + size], preferred_element_type=jnp.float32)
        u = jnp.dot(x[...], up[:, at : at + size], preferred_element_type=jnp.float32)
        h[:, at : at + size] = (g * jax.nn.sigmoid(g) * u).astype(jnp.bfloat16)
    for p in range(PIECES):
        arrived(second, (p + 1) * piece)
        term = jnp.dot(h[...], down[:, p * piece : (p + 1) * piece], preferred_element_type=jnp.float32)
        for row, ref, b in rows_of(gives):
            ref[b, p * cap : (p + 1) * cap, :] = term[row : row + cap].astype(ref.dtype)


def ffn(whole, others, parts, cap):
    width, hidden = whole[0].shape
    counts = [own.shape[0] for own, _, _ in parts]
    rows = GROUP * sum(counts) * cap
    cores = len(others[0]) if others else 0
    outs, aliases = [], {}
    for count in counts:
        shape = (count, PIECES * cap, width // PIECES)
        keep = jax.ShapeDtypeStruct(shape, jnp.float32)
        outs += [keep, keep, jax.ShapeDtypeStruct((2 * count, *shape[1:]), jnp.bfloat16)]
    scratch = [pltpu.VMEM((rows, width), jnp.bfloat16), pltpu.VMEM((rows, hidden), jnp.bfloat16)]
    flat = [w for ws in others for w in ws] if others else []
    if cores:
        aliases = {i: len(outs) + i for i in range(3)}
        outs += [jax.ShapeDtypeStruct(w.shape, w.dtype) for w in whole]
        scratch.append(pltpu.SemaphoreType.DMA((copy_count(cores, width, others[0][0].shape[1]),)))
    results = pl.pallas_call(
        functools.partial(ffn_kernel, cap, counts, cores),
        out_shape=outs,
        in_specs=[VMEM_SPEC] * 3 + [HBM_SPEC] * len(flat) + [VMEM_SPEC] * (3 * len(parts)),
        out_specs=[VMEM_SPEC] * len(outs),
        scratch_shapes=scratch,
        input_output_aliases=aliases,
        compiler_params=pltpu.CompilerParams(vmem_limit_bytes=FFN_VMEM),
        cost_estimate=pl.CostEstimate(
            flops=6 * rows * width * hidden, bytes_accessed=2 * cores * width * hidden, transcendentals=rows * hidden
        ),
        name="ffn",
    )(*whole, *flat, *[ref for part in parts for ref in part])
    gives = [tuple(results[3 * i : 3 * i + 3]) for i in range(len(counts))]
    return gives, results[3 * len(counts) :] or whole


def combine_kernel(experts, cap, pad, me_ref, ids_ref, weights_ref, *rest):
    parts, out_ref, gathered = rest[:experts], rest[experts], rest[experts + 1]
    rows, width = out_ref.shape
    piece = width // PIECES
    gathered[...] = jnp.zeros_like(gathered)
    for k in range(experts):
        for p in range(PIECES):
            gathered[k * pad : k * pad + cap, p * piece : (p + 1) * piece] = parts[k][p * cap : (p + 1) * cap, :]
    ids, me = ids_ref[...], me_ref[0]
    place = places(ids, me, experts, rows)
    row = lax.broadcasted_iota(jnp.int32, (pad, rows), 0)
    weights = jnp.transpose(weights_ref[...])
    total = jnp.zeros((rows, width), jnp.float32)
    for pick in range(2):
        onehot = [
            jnp.where((row == place[k : k + 1, :]) & (ids[pick : pick + 1, :] == (me ^ k)), 1.0, 0.0)
            for k in range(experts)
        ]
        onehot = jnp.concatenate(onehot, 0).astype(jnp.bfloat16)
        dims = (((0,), (0,)), ((), ()))
        chosen = lax.dot_general(onehot, gathered[...], dims, preferred_element_type=jnp.float32)
        total = total + chosen * weights[:, pick : pick + 1]
    out_ref[...] = total.astype(jnp.bfloat16)


def combine(me, ids, weights, parts, cap, width):
    experts, rows = len(parts), ids.shape[1]
    pad = -(-cap // 16) * 16
    return pl.pallas_call(
        functools.partial(combine_kernel, experts, cap, pad),
        out_shape=jax.ShapeDtypeStruct((rows, width), jnp.bfloat16),
        in_specs=[pl.BlockSpec(memory_space=SMEM)] + [pl.BlockSpec(memory_space=VMEM)] * (2 + experts),
        out_specs=pl.BlockSpec(memory_space=VMEM),
        scratch_shapes=[pltpu.VMEM((experts * pad, width), jnp.bfloat16)],
        cost_estimate=pl.CostEstimate(flops=1_000_000_000, bytes_accessed=1_000_000, transcendentals=0),
        compiler_params=pltpu.CompilerParams(vmem_limit_bytes=SMALL_VMEM),
        name="combine",
    )(me, ids, weights, *parts)


def per_device(tokens, norm_gain, expert_ids, gate_weights, w_gate, w_up, w_down):
    ep_devices, n_tp = lax.axis_size("ep"), lax.axis_size("tp")
    local_rows, width = tokens.shape
    picks = expert_ids.shape[1]
    experts = ep_devices // GROUP
    cap = max(2, min(local_rows, local_rows * picks * 4 // (3 * experts)))

    def shift(value, bits):
        return lax.ppermute(value, "ep", [(i, i ^ bits) for i in range(ep_devices)])

    def side(value, near):
        turn = []
        for i in range(ep_devices):
            for c in range(n_tp):
                bits = 1 if near == (c % 2 == 0) else 2
                turn.append((i * n_tp + c, (i ^ bits) * n_tp + c))
        return lax.ppermute(value, ("ep", "tp"), turn)

    def across(value):
        turns = [[(i, (i + s) % n_tp) for i in range(n_tp)] for s in range(1, n_tp)]
        return [lax.ppermute(value, "tp", turn) for turn in turns]

    def members(classes):
        return [k for k in range(experts) if k % 4 in classes]

    def joined(arrays):
        return arrays[0] if len(arrays) == 1 else jnp.concatenate(arrays)

    me = (lax.axis_index("ep") // GROUP).astype(jnp.int32).reshape(1)
    others = [across(w) for w in (w_gate, w_up, w_down)]
    blocks = pack(me, tokens, norm_gain, expert_ids.T, experts, cap)
    whole = load(w_gate, w_up, w_down, n_tp)

    taken = {}
    for g, classes in enumerate(TAKE):
        own = [shift(blocks[k], k * GROUP) if k else blocks[k] for k in members(classes)]
        own = jnp.stack(own)
        near = side(own, True)
        taken[g] = own, near, side(jnp.concatenate([own, near]), False)
    given = {}
    for groups in WORK:
        gives, whole = ffn(whole, others, [taken[g] for g in groups], cap)
        others = None
        given.update(zip(groups, gives))
    returned = [None] * experts
    for groups in GIVE:
        sizes = [len(members(TAKE[g])) for g in groups]
        got = side(joined([given[g][2] for g in groups]), False).astype(jnp.float32)
        mine, others_part, at = [], [], 0
        for n in sizes:
            mine.append(got[at : at + n])
            others_part.append(got[at + n : at + 2 * n])
            at += 2 * n
        last = joined([(given[g][1] + part).astype(jnp.bfloat16) for g, part in zip(groups, others_part)])
        last = side(last, True).astype(jnp.float32)
        at = 0
        for g, n, part in zip(groups, sizes, mine):
            total = (given[g][0] + part + last[at : at + n]).astype(jnp.bfloat16)
            at += n
            for j, k in enumerate(members(TAKE[g])):
                returned[k] = shift(total[j], k * GROUP) if k else total[j]
    return combine(me, expert_ids.T, gate_weights.T, returned, cap, width)


def solution(mesh):
    in_specs = (
        P(("grp", "ep", "tp"), None),
        P(),
        P(("grp", "ep", "tp"), None),
        P(("grp", "ep", "tp"), None),
        P(None, ("ep", "tp")),
        P(None, ("ep", "tp")),
        P(("ep", "tp"), None),
    )
    out_specs = P(("grp", "ep", "tp"), None)

    return jax.shard_map(per_device, mesh=mesh, in_specs=in_specs, out_specs=out_specs, check_vma=False)
```
